32 devices in a mesh: fs: 8 (over z, x), tp: 4 (over y, core).
Axes of the slice: x: 2, y: 2, z: 4, core: 2. Of those that a mesh axis runs over, the one named last changes fastest.
Arguments:
- prompt_tokens: bfloat16 [6144, 2048], P('fs', 'tp'), may hold values from -6 to 6
- norm_gain: float32 [2048], P('fs'), may hold values from 0.1 to 1.9
- up_master: float32 [2048, 4096], P('fs', 'tp'), may hold values from -6 to 6
- down_master: float32 [2048, 4096], P('fs', 'tp'), may hold values from -6 to 6
Outputs:
- serve_up: bfloat16 [2048, 4096], P(None, 'tp')
- serve_down: bfloat16 [2048, 4096], P(None, 'tp')
- mixed: bfloat16 [6144, 2048], P('fs', 'tp')
The draws below stay inside these ranges and needn't reach their ends.
All inputs are finite; a program needn't handle non-finite values.
Results may differ from the reference program's by a relative error of at most 0.009.
Values may be sent and summed in bfloat16 or wider, within the bound.
No kernel may reach another device: no remote copies, remote signals or barrier semaphores. Data moves between devices by JAX's collectives and lax.ppermute only.
A program may use at most 64 MiB of HBM per device.

```python
import jax
import jax.numpy as jnp
from jax import lax

D = 2048
FF = 4096
TOK_DEV = 768
TOKENS = 6144
N_FS = 8
N_TP = 4


def steps_of(own_key, extent, shards, low, high):
    level = 1.0
    for dim, shards_of in shards:
        heights = jax.random.uniform(jax.random.fold_in(jax.random.fold_in(own_key, 6), dim), (shards_of,), jnp.float32, low / len(shards), high / len(shards))
        level = level * jnp.repeat(jnp.exp(heights), extent[dim] // shards_of).reshape((-1,) + (1,) * (len(extent) - 1 - dim))
    return level


def centred(own_key, shape, deviation, most, split=(), held_as=jnp.bfloat16):
    values = jax.random.normal(own_key, shape, jnp.float32) * deviation
    if len(split) > 0:
        values = steps_of(own_key, shape, split, -0.22, 0.18) * values
    return jnp.clip(values, min=-most, max=most).astype(held_as)


def setup_inputs(seed: int = 0) -> dict:
    arg_keys = jax.random.split(jax.random.key(seed), 5)
    prompt_tokens = centred(arg_keys[0], (TOKENS, D), 1.0, 6.0, ((0, 8), (1, 4)))
    norm_gain = jnp.clip(1.0 + 0.18 * jax.random.normal(arg_keys[1], (D,), jnp.float32), 0.1, 1.9)
    up_master = centred(arg_keys[2], (D, FF), 1.0, 6.0, ((0, 8), (1, 4)), jnp.float32)
    down_master = centred(arg_keys[3], (D, FF), 1.0, 6.0, ((0, 8), (1, 4)), jnp.float32)
    return dict(prompt_tokens=prompt_tokens, norm_gain=norm_gain, up_master=up_master, down_master=down_master)


def reference(prompt_tokens, norm_gain, up_master, down_master):
    serve_up = (norm_gain[:, None] * up_master).astype(jnp.bfloat16)
    serve_down = down_master.astype(jnp.bfloat16)
    group = FF // N_TP
    blocks = prompt_tokens.reshape(N_FS, TOK_DEV, D)

    def one_block(block):
        wide = block.astype(jnp.float32)
        normed = (wide * lax.rsqrt(lax.optimization_barrier(jnp.mean(wide * wide, axis=1, keepdims=True)) + 1e-05)).astype(jnp.bfloat16)
        hidden = jnp.dot(normed, serve_up, preferred_element_type=jnp.float32) * D ** (-0.5)
        act = jnp.square(jax.nn.relu(hidden)).astype(jnp.bfloat16)
        total = jnp.zeros((TOK_DEV, D), jnp.float32)
        for index in range(N_TP):
            act_part = act[:, index * group:(index + 1) * group]
            down_part = serve_down[:, index * group:(index + 1) * group]
            partial_value = lax.dot_general(act_part, down_part, (((1,), (1,)), ((), ())), preferred_element_type=jnp.float32) * FF ** (-0.5)
            total = total + partial_value.astype(jnp.bfloat16).astype(jnp.float32)
        return total.astype(jnp.bfloat16)
    mixed = lax.map(one_block, blocks).reshape(TOKENS, D)
    return (serve_up, serve_down, mixed)
```

```python
import jax
import jax.numpy as jnp
from jax import lax
from jax.sharding import PartitionSpec as P

F32, BF16 = jnp.float32, jnp.bfloat16
ROWS_OF_BOTH = (((1,), (1,)), ((), ()))
Z, X, Y, C = 4, 2, 2, 2


def plain(prompt_tokens, norm_gain, up_master, down_master):
    up_folded = (norm_gain[:, None] * up_master).astype(BF16)
    down_cast = down_master.astype(BF16)
    wide = lax.all_gather(prompt_tokens, "tp", axis=1, tiled=True).astype(F32)
    width = wide.shape[1]
    hidden_units = up_master.shape[1] * lax.axis_size("tp")
    normed = (wide * lax.rsqrt(jnp.mean(wide * wide, axis=1, keepdims=True) + 1e-05)).astype(BF16)
    serve_up = lax.all_gather(up_folded, "fs", axis=0, tiled=True)
    serve_down = lax.all_gather(down_cast, "fs", axis=0, tiled=True)
    hidden = jnp.dot(normed, serve_up, preferred_element_type=F32)
    act = jnp.square(jax.nn.relu(hidden * width ** (-0.5))).astype(BF16)
    product = lax.dot_general(act, serve_down, ROWS_OF_BOTH, preferred_element_type=F32)
    partial = (product * hidden_units ** (-0.5)).astype(BF16)
    mixed = lax.psum_scatter(partial, "tp", scatter_dimension=1, tiled=True)
    return serve_up, serve_down, mixed


def pairs(target):
    out = []
    for z in range(Z):
        for x in range(X):
            to = target(z, x)
            if to is not None:
                out.append((z * X + x, to[0] * X + to[1]))
    return out


OTHER_X = pairs(lambda z, x: (z, 1 - x))
NEAR_Z = pairs(lambda z, x: (z ^ 1, x))
MID_Z = pairs(lambda z, x: (3 - z, x) if z in (1, 2) else None)
OUT_Z = pairs(lambda z, x: (z ^ 1, x) if z in (1, 2) else None)
OTHER_Y = [(k, k ^ 2) for k in range(Y * C)]
OTHER_C = [(k, k ^ 1) for k in range(Y * C)]


def to_plane(stage):
    out = []
    for i in range(Z * X):
        to = (i // X) // 2 if stage == 0 else 1 - (i // X) // 2
        for c in range(C):
            out.append((i * Y * C + (1 - to) * C + c, i * Y * C + to * C + c))
    return out


def gathered(own, rows, z, x):
    hop = lambda v, p: lax.ppermute(v, "fs", p)
    inner = (z == 1) | (z == 2)
    x0 = hop(own, OTHER_X)
    a1 = hop(own, NEAR_Z)
    b1 = hop(own, MID_Z)
    b2 = hop(a1, MID_Z)
    a2 = hop(b1, OUT_Z)
    a3 = hop(b2, OUT_Z)
    c1 = jnp.where(inner, b1, a2)
    c2 = jnp.where(inner, b2, a3)
    x1, x2, x3 = hop(a1, OTHER_X), hop(c1, OTHER_X), hop(c2, OTHER_X)
    low = z < 2
    z1 = z ^ 1
    z2 = jnp.where(low, 2, 1)
    z3 = jnp.where(low, 3, 0)
    whole = jnp.zeros((rows * Z * X, own.shape[1]), own.dtype)
    for part, at, side in ((own, z, x), (x0, z, 1 - x), (a1, z1, x), (x1, z1, 1 - x), (c1, z2, x), (x2, z2, 1 - x), (c2, z3, x), (x3, z3, 1 - x)):
        whole = lax.dynamic_update_slice(whole, part, ((at * X + side) * rows, 0))
    return whole


def shards(prompt_tokens, norm_gain, up_master, down_master):
    i, k = lax.axis_index("fs"), lax.axis_index("tp")
    z, x, y, c = i // X, i % X, k // C, k % C
    rows, block = up_master.shape[0], prompt_tokens.shape[1]
    width = block * lax.axis_size("tp")
    hidden_units = up_master.shape[1] * lax.axis_size("tp")
    up_own = (norm_gain[:, None] * up_master).astype(BF16)
    down_own = down_master.astype(BF16)

    far = lax.ppermute(prompt_tokens, "tp", OTHER_Y)
    near = lax.ppermute(prompt_tokens, "tp", OTHER_C)
    cross = lax.ppermute(far, "tp", OTHER_C)
    parts = ((prompt_tokens, k), (near, k ^ 1), (far, k ^ 2), (cross, k ^ 3))
    total = sum(jnp.sum(jnp.square(p.astype(F32)), axis=1, keepdims=True) for p, _ in parts)
    scale = lax.rsqrt(total / width + 1e-05)
    normed = jnp.zeros((prompt_tokens.shape[0], width), BF16)
    for p, at in parts:
        normed = lax.dynamic_update_slice(normed, (p.astype(F32) * scale).astype(BF16), (0, at * block))

    serve_up = gathered(up_own, rows, z, x)
    serve_down = gathered(down_own, rows, z, x)
    hidden = jnp.dot(normed, serve_up, preferred_element_type=F32)
    act = jnp.square(jax.nn.relu(hidden * width ** (-0.5))).astype(BF16)

    def share(j):
        mine = lax.dynamic_slice(serve_down, (j * block, 0), (block, serve_down.shape[1]))
        product = lax.dot_general(act, mine, ROWS_OF_BOTH, preferred_element_type=F32)
        return (product * hidden_units ** (-0.5)).astype(BF16)

    sums = []
    for stage in range(2):
        plane = z // 2 if stage == 0 else 1 - z // 2
        sent = lax.ppermute(share(plane * C + 1 - c), "tp", OTHER_C)
        chip = share(plane * C + c).astype(F32) + sent.astype(F32)
        got = lax.ppermute(chip.astype(BF16), ("fs", "tp"), to_plane(stage))
        sums.append(chip + got.astype(F32))
    mixed = jnp.where(y == z // 2, sums[0], sums[1]).astype(BF16)
    return serve_up, serve_down, mixed


def solution(mesh):
    lines = mesh.shape["fs"] == Z * X and mesh.shape["tp"] == Y * C
    return jax.shard_map(
        shards if lines else plain,
        mesh=mesh,
        in_specs=(P("fs", "tp"), P("fs"), P("fs", "tp"), P("fs", "tp")),
        out_specs=(P(None, "tp"), P(None, "tp"), P("fs", "tp")),
        check_vma=False,
    )
```
